32 devices in a mesh: sp: 8 (over z, y), dp: 4 (over x, core).
Axes of the slice: x: 2, y: 2, z: 4, core: 2. Of those that a mesh axis runs over, the one named last changes fastest.
Arguments:
- layer_input: bfloat16 [4, 1024, 2048], P('dp', 'sp'), may hold values from -0.0390625 to 0.0390625
- queries: bfloat16 [4, 1024, 2048], P('dp', 'sp'), may hold values from -6 to 6
- key_vectors: bfloat16 [4, 1024, 2048], P('dp', 'sp'), may hold values from -6 to 6
- values: bfloat16 [4, 1024, 4096], P('dp', 'sp'), may hold values from -6 to 6
- cotangent: bfloat16 [4, 1024, 4096], P('dp', 'sp'), may hold values from -0.3125 to 0.3125
- log_decay: float32 [4, 16, 1024], P('dp', 'sp'), may hold values from -3 to 0
- key_weight: bfloat16 [2048, 2048], P('dp'), may hold values from -0.125 to 0.125
Outputs:
- grad_query: bfloat16 [4, 1024, 2048], P('dp', 'sp')
- grad_value: bfloat16 [4, 1024, 4096], P('dp', 'sp')
- grad_input: bfloat16 [4, 1024, 2048], P('dp', 'sp')
- grad_key_weight: float32 [2048, 2048], P('dp')
The draws below stay inside these ranges and needn't reach their ends.
All inputs are finite; a program needn't handle non-finite values.
Results may differ from the reference program's by a relative error of at most 0.012.
Values may be sent and summed in bfloat16 or wider, within the bound.
A program may use at most 128 MiB of HBM per device.

```python
import jax
import jax.numpy as jnp
from jax import lax

D = 2048
HEADS = 8
DK = 256
DV = 512
BLOCK = 128
TOK_DEV = 128
HEAD_DIRECTIONS = 16
SEQUENCE_LENGTH = 1024
SEQUENCE_COUNT = 4
HK = 2048
HV = 4096


def draw_log_decay(key, part):
    parallel_lanes = jax.random.split(jax.random.fold_in(key, 71), 6)
    fast_share = 0.5
    is_fast = jax.random.uniform(parallel_lanes[0], (SEQUENCE_COUNT, HEAD_DIRECTIONS, 1)) < fast_share
    fast_rate = jnp.exp(jax.random.uniform(parallel_lanes[1], (SEQUENCE_COUNT, HEAD_DIRECTIONS, 1), jnp.float32, jnp.log(2.0), jnp.log(6.0))) / BLOCK
    slow_rate = jnp.ones((SEQUENCE_COUNT, HEAD_DIRECTIONS, 1), jnp.float32) / SEQUENCE_LENGTH
    baseline_decay_rate = jnp.where(is_fast, fast_rate, slow_rate)
    block_multiplier = jnp.exp(jax.random.uniform(parallel_lanes[2], (SEQUENCE_COUNT, HEAD_DIRECTIONS, SEQUENCE_LENGTH // TOK_DEV), jnp.float32, jnp.log(0.5), jnp.log(2.0)))
    block_multiplier = jnp.repeat(block_multiplier, TOK_DEV, axis=2)
    decay_jitter = jax.random.uniform(parallel_lanes[3], (SEQUENCE_COUNT, HEAD_DIRECTIONS, SEQUENCE_LENGTH), jnp.float32, 0.5, 1.5)
    group_position = jax.random.randint(parallel_lanes[4], (SEQUENCE_COUNT, HEAD_DIRECTIONS, 2), 0, SEQUENCE_LENGTH)
    group_depth = jnp.log(jax.random.uniform(parallel_lanes[5], (SEQUENCE_COUNT, HEAD_DIRECTIONS, 2), jnp.float32, 0.5, 0.8))
    position_slots = jnp.arange(SEQUENCE_LENGTH)[None, None, None, :]
    token_groups = jnp.sum(jnp.where(position_slots == group_position[..., None], group_depth[..., None], 0.0), axis=2)
    return (-baseline_decay_rate * block_multiplier * decay_jitter + token_groups).astype(jnp.float32)


def with_spikes(drawn, own_key, source, target, blocks, factor):
    def block_of(axis_at):
        return (jnp.arange(drawn.shape[axis_at]) // (drawn.shape[axis_at] // blocks)).reshape((-1,) + (1,) * (drawn.ndim - 1 - axis_at))

    near = jax.random.permutation(own_key, blocks)[block_of(target)]
    other_side = (block_of(target) + blocks // 2) % blocks
    return jnp.where((block_of(source) == near) | (block_of(source) == other_side), factor * drawn, drawn)


def level_of(rng, shape, cuts, least, largest):
    loudness, own = 1.0, jax.random.fold_in(rng, 6)
    for dim, shards_of in cuts:
        draws = jnp.exp(jax.random.uniform(jax.random.fold_in(own, dim), (shards_of,), jnp.float32, least / len(cuts), largest / len(cuts)))
        loudness = loudness * jnp.repeat(draws, shape[dim] // shards_of).reshape([-1 if axis == dim else 1 for axis in range(len(shape))])
    return loudness


def scatter_about(rng, dims, scale, reach, cuts=(), held_as=jnp.bfloat16):
    gain = level_of(rng, dims, cuts, -0.22, 0.18) if cuts else 1.0
    drawn = jax.random.normal(rng, dims, jnp.float32) * scale * gain
    return jnp.minimum(jnp.maximum(drawn, -reach), reach).astype(held_as)


def heavy_noise(own_key, shape, width, most, shards, heavy, kind=jnp.bfloat16):
    values = width * jax.random.normal(own_key, shape, jnp.float32)
    if shards:
        values = values * level_of(own_key, shape, shards, -0.22, 0.18)
    return jnp.clip(with_spikes(values, jax.random.fold_in(own_key, 3), *heavy), -most, most).astype(kind)


def setup_inputs(seed: int = 0) -> dict:
    streams_of = jax.random.split(jax.random.key(seed), 8)
    layer_input = heavy_noise(streams_of[0], (SEQUENCE_COUNT, SEQUENCE_LENGTH, D), 0.005, 0.0390625, ((0, 4), (1, 8)), (1, 2, 8, 2.0))
    queries = scatter_about(streams_of[1], (SEQUENCE_COUNT, SEQUENCE_LENGTH, HK), 1.0, 6.0, ((0, 4), (1, 8)))
    key_vectors = scatter_about(streams_of[2], (SEQUENCE_COUNT, SEQUENCE_LENGTH, HK), 1.0, 6.0, ((0, 4), (1, 8)))
    values = scatter_about(streams_of[3], (SEQUENCE_COUNT, SEQUENCE_LENGTH, HV), 1.0, 6.0, ((0, 4), (1, 8)))
    cotangent = scatter_about(streams_of[4], (SEQUENCE_COUNT, SEQUENCE_LENGTH, HV), 0.05, 0.3125, ((0, 4), (1, 8)))
    log_decay = draw_log_decay(jax.random.fold_in(streams_of[7], 71), 0)
    key_weight = scatter_about(streams_of[6], (D, HK), D ** -0.5, 0.125, ((0, 4),))
    return {"layer_input": layer_input, "queries": queries, "key_vectors": key_vectors, "values": values, "cotangent": cotangent, "log_decay": log_decay, "key_weight": key_weight}


def unit_backward(query_rows, key_rows, value_rows, grad_rows, decay_rows, strict):
    length, key_width = query_rows.shape
    value_width = value_rows.shape[1]
    blocks = length // BLOCK
    scaling = key_width ** -0.5
    query_blk = query_rows.reshape(blocks, BLOCK, key_width)
    key_blk = key_rows.reshape(blocks, BLOCK, key_width)
    value_blk = value_rows.reshape(blocks, BLOCK, value_width)
    grad_blk = grad_rows.reshape(blocks, BLOCK, value_width)
    within = jnp.cumsum(decay_rows.reshape(blocks, BLOCK), axis=1)
    position_slots = jnp.arange(BLOCK)
    allowed = jnp.where(strict, position_slots[None, :] < position_slots[:, None], position_slots[None, :] <= position_slots[:, None])
    spread = jnp.where(allowed, within[:, :, None] - within[:, None, :], 0.0)
    weights = jnp.where(allowed, jnp.exp(spread), 0.0) * scaling
    raw_scores = jnp.einsum("nid,njd->nij", query_blk, key_blk, preferred_element_type=jnp.float32)
    scores = (raw_scores * weights).astype(jnp.bfloat16)
    raw_grads = jnp.einsum("niv,njv->nij", grad_blk, value_blk, preferred_element_type=jnp.float32)
    grad_scores = (raw_grads * weights).astype(jnp.bfloat16)
    value_inner = jnp.einsum("nij,niv->njv", scores, grad_blk, preferred_element_type=jnp.float32)
    query_inner = jnp.einsum("nij,njd->nid", grad_scores, key_blk, preferred_element_type=jnp.float32)
    key_inner = jnp.einsum("nij,nid->njd", grad_scores, query_blk, preferred_element_type=jnp.float32)
    ending = within[:, -1:]
    query_scale = jnp.exp(within) * scaling
    key_scale = jnp.exp(ending - within)
    carry_decay = jnp.exp(ending[:, 0])
    query_dec = (query_blk * query_scale[:, :, None]).astype(jnp.bfloat16)
    key_dec = (key_blk * key_scale[:, :, None]).astype(jnp.bfloat16)
    contract = (((0,), (0,)), ((), ()))

    def advance(memory, inputs):
        key_b, value_b, factor = inputs
        before = memory.astype(jnp.bfloat16)
        memory = factor * memory + lax.dot_general(key_b, value_b, contract, preferred_element_type=jnp.float32)
        return memory, before

    start_state = jnp.zeros((key_width, value_width), jnp.float32)
    _, states_before = lax.scan(advance, start_state, (key_dec, value_blk, carry_decay))

    def retreat(later, inputs):
        query_b, grad_b, factor = inputs
        after = later.astype(jnp.bfloat16)
        later = factor * later + lax.dot_general(query_b, grad_b, contract, preferred_element_type=jnp.float32)
        return later, after

    _, state_grads = lax.scan(retreat, start_state, (query_dec, grad_blk, carry_decay), reverse=True)
    query_carried = jnp.einsum("niv,ndv->nid", grad_blk, states_before, preferred_element_type=jnp.float32)
    key_carried = jnp.einsum("njv,ndv->njd", value_blk, state_grads, preferred_element_type=jnp.float32)
    value_carried = jnp.einsum("njd,ndv->njv", key_dec, state_grads, preferred_element_type=jnp.float32)
    grad_q = query_inner + query_carried * query_scale[:, :, None]
    grad_k = key_inner + key_carried * key_scale[:, :, None]
    grad_v = value_inner + value_carried
    return (grad_q.reshape(length, key_width), grad_k.reshape(length, key_width),
            grad_v.reshape(length, value_width))


def unit_grads(query_rows, key_rows, value_rows, grad_rows, decay_rows, backward):
    def orient(array):
        return jnp.where(backward, jnp.flip(array, 0), array)

    gradients = unit_backward(orient(query_rows), orient(key_rows), orient(value_rows),
                              orient(grad_rows), orient(decay_rows), backward)
    return tuple(orient(single).astype(jnp.bfloat16) for single in gradients)


def reference(layer_input, queries, key_vectors, values, cotangent, log_decay, key_weight):
    def one_sequence(inputs):
        rows_in, query_seq, key_seq, value_seq, grad_seq, decay_seq = inputs
        length = query_seq.shape[0]
        query_heads = query_seq.reshape(length, HEADS, DK)
        key_heads = key_seq.reshape(length, HEADS, DK)
        value_heads = value_seq.reshape(length, HEADS, DV)
        grad_heads = grad_seq.reshape(length, HEADS, DV)
        query_list, key_list, value_list = [], [], []
        for head_index in range(HEADS):
            halves = [unit_grads(query_heads[:, head_index], key_heads[:, head_index], value_heads[:, head_index],
                                 grad_heads[:, head_index], decay_seq[2 * head_index + direction], direction == 1)
                      for direction in range(2)]
            paired = [(halves[0][slot].astype(jnp.float32) + halves[1][slot].astype(jnp.float32)).astype(jnp.bfloat16)
                      for slot in range(3)]
            query_list.append(paired[0])
            key_list.append(paired[1])
            value_list.append(paired[2])
        grad_query = jnp.concatenate(query_list, axis=1)
        grad_key = jnp.concatenate(key_list, axis=1)
        grad_value = jnp.concatenate(value_list, axis=1)
        grad_input = jnp.dot(grad_key, key_weight.T, preferred_element_type=jnp.float32).astype(jnp.bfloat16)
        local_term = jnp.dot(rows_in.T, grad_key, preferred_element_type=jnp.float32)
        return grad_query, grad_value, grad_input, local_term

    outputs = lax.map(one_sequence, (layer_input, queries, key_vectors, values, cotangent, log_decay))
    return outputs[0], outputs[1], outputs[2], jnp.sum(outputs[3], axis=0)
```

```python
import functools

import jax
import jax.numpy as jnp
from jax import lax
from jax.experimental import pallas as pl
from jax.experimental.pallas import tpu as pltpu
from jax.sharding import PartitionSpec as P

HEADS = 8
BLOCK = 128
MESH = pl.DeviceIdType.MESH
BF16 = jnp.bfloat16
F32 = jnp.float32


def dot_nn(a, b):
    return lax.dot_general(a, b, (((1,), (0,)), ((), ())), preferred_element_type=F32)


def dot_nt(a, b):
    return lax.dot_general(a, b, (((1,), (1,)), ((), ())), preferred_element_type=F32)


def dot_tn(a, b):
    return lax.dot_general(a, b, (((0,), (0,)), ((), ())), preferred_element_type=F32)


def decay_columns(lam_ref, b):
    lam_fwd = lam_ref[0, b]
    lam_bwd = lam_ref[1, b]
    row = lax.broadcasted_iota(jnp.int32, (BLOCK, BLOCK), 0)
    col = lax.broadcasted_iota(jnp.int32, (BLOCK, BLOCK), 1)
    lower = col <= row
    c0 = jnp.sum(jnp.where(lower, lam_fwd, 0.0), axis=1, keepdims=True)
    c1 = jnp.sum(jnp.where(col >= row, lam_bwd, 0.0), axis=1, keepdims=True)
    e0 = jnp.sum(lam_fwd, axis=1, keepdims=True)
    e1 = jnp.sum(lam_bwd, axis=1, keepdims=True)
    return c0, c1, e0, e1, row, col, lower


def as_row(column, row, col):
    return jnp.sum(jnp.where(row == col, column, 0.0), axis=0, keepdims=True)


def retention_kernel(
    sp,
    q_in, k_in, v_in, g_in, lam_ref,
    q_home, k_home, v_home, k_head,
    qa, ka, va, ga,
    qacc, kacc, vacc,
    dm0, dm1, dg0, dg1,
    sm0, sg1,
    run_a, run_b,
    qh, kh, vh,
    in_send, in_recv, out_send, out_recv, local_sem, head_sem,
):
    me = lax.axis_index("sp")
    dk = qa.shape[1]
    dv = va.shape[1]
    scaling = dk ** (-0.5)
    ins = ((q_in, qa, dk), (k_in, ka, dk), (v_in, va, dv), (g_in, ga, dv))
    outs = ((qh, q_home, dk), (kh, k_home, dk), (vh, v_home, dv))

    def rows_of(b):
        return pl.ds(pl.multiple_of(b * BLOCK, BLOCK), BLOCK)

    def cols_of(b, width):
        return pl.ds(pl.multiple_of(b * width, width), width)

    locals_in = [
        pltpu.make_async_copy(src.at[:, cols_of(me, w)], dst.at[rows_of(me)], local_sem.at[t])
        for t, (src, dst, w) in enumerate(ins)
    ]
    for copy in locals_in:
        copy.start()

    barrier = pltpu.get_barrier_semaphore()
    for off in range(1, sp):
        pl.semaphore_signal(
            barrier, inc=1, device_id={"sp": lax.rem(me + off, sp)}, device_id_type=MESH
        )
    pl.semaphore_wait(barrier, sp - 1)

    def incoming(t, off):
        src, dst, w = ins[t]
        peer = lax.rem(me + off, sp)
        return pltpu.make_async_remote_copy(
            src_ref=src.at[:, cols_of(peer, w)],
            dst_ref=dst.at[rows_of(me)],
            send_sem=in_send.at[t, off],
            recv_sem=in_recv.at[t, off],
            device_id={"sp": peer},
            device_id_type=MESH,
        )

    for off in range(1, sp):
        for t in range(4):
            incoming(t, off).start()

    def local_part(b):
        rows = rows_of(b)
        q, k, v, g = qa[rows, :], ka[rows, :], va[rows, :], ga[rows, :]
        c0, c1, e0, e1, row, col, lower = decay_columns(lam_ref, b)
        spread = jnp.where(lower, c0 - as_row(c0, row, col), c1 - as_row(c1, row, col))
        weights = jnp.exp(spread) * scaling
        scores = (dot_nt(q, k) * weights).astype(BF16)
        grads = (dot_nt(g, v) * weights).astype(BF16)
        qacc[rows, :] = dot_nn(grads, k)
        kacc[rows, :] = dot_tn(grads, q)
        vacc[rows, :] = dot_tn(scores, g)
        qf, kf = q.astype(F32), k.astype(F32)
        dm0[b] = dot_tn((kf * jnp.exp(e0 - c0)).astype(BF16), v)
        dm1[b] = dot_tn((kf * jnp.exp(e1 - c1)).astype(BF16), v)
        dg0[b] = dot_tn((qf * (jnp.exp(c0) * scaling)).astype(BF16), g)
        dg1[b] = dot_tn((qf * (jnp.exp(c1) * scaling)).astype(BF16), g)

    for copy in locals_in:
        copy.wait()
    local_part(me)

    def arrive(off, carry):
        for t in range(4):
            incoming(t, off).wait_recv()
        local_part(lax.rem(me + sp - off, sp))
        return carry

    lax.fori_loop(1, sp, arrive, 0)

    run_a[...] = jnp.zeros_like(run_a)
    run_b[...] = jnp.zeros_like(run_b)

    def forward(b, carry):
        e0 = jnp.exp(jnp.sum(lam_ref[0, b], axis=1, keepdims=True))
        e1 = jnp.exp(jnp.sum(lam_ref[1, b], axis=1, keepdims=True))
        m0 = run_a[...]
        sm0[b] = m0.astype(BF16)
        run_a[...] = e0 * m0 + dm0[b]
        g1 = run_b[...]
        sg1[b] = g1.astype(BF16)
        run_b[...] = e1 * g1 + dg1[b]
        return carry

    lax.fori_loop(0, sp, forward, 0)

    run_a[...] = jnp.zeros_like(run_a)
    run_b[...] = jnp.zeros_like(run_b)

    def outgoing(t, b, source):
        src, dst, w = outs[t]
        return pltpu.make_async_remote_copy(
            src_ref=src.at[rows_of(b)],
            dst_ref=dst.at[:, cols_of(source, w)],
            send_sem=out_send.at[t, b],
            recv_sem=out_recv.at[t, source],
            device_id={"sp": b},
            device_id_type=MESH,
        )

    def local_out(t):
        src, dst, w = outs[t]
        return pltpu.make_async_copy(src.at[rows_of(me)], dst.at[:, cols_of(me, w)], local_sem.at[t])

    def backward(step, carry):
        b = sp - 1 - step
        rows = rows_of(b)
        k, v, g = ka[rows, :], va[rows, :], ga[rows, :]
        c0, c1, e0, e1, _, _, _ = decay_columns(lam_ref, b)
        kf = k.astype(F32)
        ks0, ks1 = jnp.exp(e0 - c0), jnp.exp(e1 - c1)
        m0, g1 = sm0[b], sg1[b]
        g0, m1 = run_a[...].astype(BF16), run_b[...].astype(BF16)
        qh[rows, :] = (
            qacc[rows, :]
            + dot_nt(g, m0) * (jnp.exp(c0) * scaling)
            + dot_nt(g, m1) * (jnp.exp(c1) * scaling)
        ).astype(BF16)
        kh[rows, :] = (kacc[rows, :] + dot_nt(v, g0) * ks0 + dot_nt(v, g1) * ks1).astype(BF16)
        vh[rows, :] = (
            vacc[rows, :]
            + dot_nn((kf * ks0).astype(BF16), g0)
            + dot_nn((kf * ks1).astype(BF16), g1)
        ).astype(BF16)
        run_a[...] = jnp.exp(e0) * run_a[...] + dg0[b]
        run_b[...] = jnp.exp(e1) * run_b[...] + dm1[b]

        @pl.when(b != me)
        def _():
            for t in (1, 0, 2):
                outgoing(t, b, me).start()

        @pl.when(b == me)
        def _():
            for t in range(3):
                local_out(t).start()

        return carry

    lax.fori_loop(0, sp, backward, 0)

    head_copy = pltpu.make_async_copy(kh, k_head, head_sem)
    head_copy.start()

    for t in range(3):
        local_out(t).wait()

    for off in range(1, sp):
        for t in range(4):
            incoming(t, off).wait_send()

    def settle(off, carry):
        peer = lax.rem(me + off, sp)
        for t in range(3):
            outgoing(t, peer, peer).wait()
        return carry

    lax.fori_loop(1, sp, settle, 0)
    head_copy.wait()


def retention_by_head(queries, key_vectors, values, cotangent, log_decay, sp):
    tokens, hk = queries.shape
    hv = values.shape[1]
    length = tokens * sp
    dk, dv = hk // HEADS, hv // HEADS
    lam = log_decay.reshape(2, sp, 1, BLOCK)
    anyspace = pl.BlockSpec(memory_space=pl.ANY)
    return pl.pallas_call(
        functools.partial(retention_kernel, sp),
        out_shape=(
            jax.ShapeDtypeStruct((tokens, hk), BF16),
            jax.ShapeDtypeStruct((tokens, hk), BF16),
            jax.ShapeDtypeStruct((tokens, hv), BF16),
            jax.ShapeDtypeStruct((length, dk), BF16),
        ),
        in_specs=[anyspace] * 4 + [pl.BlockSpec(memory_space=pltpu.VMEM)],
        out_specs=(anyspace,) * 4,
        scratch_shapes=[
            pltpu.VMEM((length, dk), BF16),
            pltpu.VMEM((length, dk), BF16),
            pltpu.VMEM((length, dv), BF16),
            pltpu.VMEM((length, dv), BF16),
            pltpu.VMEM((length, dk), F32),
            pltpu.VMEM((length, dk), F32),
            pltpu.VMEM((length, dv), F32),
            pltpu.VMEM((sp, dk, dv), F32),
            pltpu.VMEM((sp, dk, dv), F32),
            pltpu.VMEM((sp, dk, dv), F32),
            pltpu.VMEM((sp, dk, dv), F32),
            pltpu.VMEM((sp, dk, dv), BF16),
            pltpu.VMEM((sp, dk, dv), BF16),
            pltpu.VMEM((dk, dv), F32),
            pltpu.VMEM((dk, dv), F32),
            pltpu.VMEM((length, dk), BF16),
            pltpu.VMEM((length, dk), BF16),
            pltpu.VMEM((length, dv), BF16),
            pltpu.SemaphoreType.DMA((4, sp)),
            pltpu.SemaphoreType.DMA((4, sp)),
            pltpu.SemaphoreType.DMA((3, sp)),
            pltpu.SemaphoreType.DMA((3, sp)),
            pltpu.SemaphoreType.DMA((4,)),
            pltpu.SemaphoreType.DMA(()),
        ],
        compiler_params=pltpu.CompilerParams(
            collective_id=0, has_side_effects=True, vmem_limit_bytes=50 * 1024 * 1024
        ),
        cost_estimate=pl.CostEstimate(
            flops=6_000_000_000, bytes_accessed=150_000_000, transcendentals=0
        ),
    )(queries, key_vectors, values, cotangent, lam)


def shards_by_head(sp, layer_input, queries, key_vectors, values, cotangent, log_decay, key_weight):
    all_weight = lax.all_gather(key_weight, "dp", axis=0, tiled=True)
    all_rows = lax.all_gather(layer_input[0], "sp", axis=0, tiled=True)
    grad_query, grad_key, grad_value, key_head = retention_by_head(
        queries[0], key_vectors[0], values[0], cotangent[0], log_decay[0], sp
    )
    partial = lax.dot_general(
        all_rows, key_head, (((0,), (0,)), ((), ())), preferred_element_type=F32
    ).astype(BF16)
    summed = lax.psum_scatter(partial, "dp", scatter_dimension=0, tiled=True)
    grad_input = lax.dot_general(
        grad_key, all_weight, (((1,), (1,)), ((), ())), preferred_element_type=F32
    ).astype(BF16)
    grad_weight = lax.all_gather(summed, "sp", axis=1, tiled=True).astype(F32)
    return (grad_query[None], grad_value[None], grad_input[None], grad_weight)


def unit_backward(query_rows, key_rows, value_rows, grad_rows, decay_rows, strict):
    length, key_width = query_rows.shape
    value_width = value_rows.shape[1]
    blocks = length // BLOCK
    scaling = key_width ** (-0.5)
    query_blk = query_rows.reshape(blocks, BLOCK, key_width)
    key_blk = key_rows.reshape(blocks, BLOCK, key_width)
    value_blk = value_rows.reshape(blocks, BLOCK, value_width)
    grad_blk = grad_rows.reshape(blocks, BLOCK, value_width)
    within = jnp.cumsum(decay_rows.reshape(blocks, BLOCK), axis=1)
    position_slots = jnp.arange(BLOCK)
    allowed = jnp.where(
        strict,
        position_slots[None, :] < position_slots[:, None],
        position_slots[None, :] <= position_slots[:, None],
    )
    spread = jnp.where(allowed, within[:, :, None] - within[:, None, :], 0.0)
    weights = jnp.where(allowed, jnp.exp(spread), 0.0) * scaling
    raw_scores = jnp.einsum("nid,njd->nij", query_blk, key_blk, preferred_element_type=jnp.float32)
    scores = (raw_scores * weights).astype(jnp.bfloat16)
    raw_grads = jnp.einsum("niv,njv->nij", grad_blk, value_blk, preferred_element_type=jnp.float32)
    grad_scores = (raw_grads * weights).astype(jnp.bfloat16)
    value_inner = jnp.einsum("nij,niv->njv", scores, grad_blk, preferred_element_type=jnp.float32)
    query_inner = jnp.einsum(
        "nij,njd->nid", grad_scores, key_blk, preferred_element_type=jnp.float32
    )
    key_inner = jnp.einsum(
        "nij,nid->njd", grad_scores, query_blk, preferred_element_type=jnp.float32
    )
    ending = within[:, -1:]
    query_scale = jnp.exp(within) * scaling
    key_scale = jnp.exp(ending - within)
    carry_decay = jnp.exp(ending[:, 0])
    query_dec = (query_blk * query_scale[:, :, None]).astype(jnp.bfloat16)
    key_dec = (key_blk * key_scale[:, :, None]).astype(jnp.bfloat16)
    contract = (((0,), (0,)), ((), ()))

    def advance(memory, inputs):
        key_b, value_b, factor = inputs
        before = memory.astype(jnp.bfloat16)
        memory = factor * memory + lax.dot_general(
            key_b, value_b, contract, preferred_element_type=jnp.float32
        )
        return (memory, before)

    start_state = jnp.zeros((key_width, value_width), jnp.float32)
    _, states_before = lax.scan(advance, start_state, (key_dec, value_blk, carry_decay))

    def retreat(later, inputs):
        query_b, grad_b, factor = inputs
        after = later.astype(jnp.bfloat16)
        later = factor * later + lax.dot_general(
            query_b, grad_b, contract, preferred_element_type=jnp.float32
        )
        return (later, after)

    _, state_grads = lax.scan(
        retreat, start_state, (query_dec, grad_blk, carry_decay), reverse=True
    )
    query_carried = jnp.einsum(
        "niv,ndv->nid", grad_blk, states_before, preferred_element_type=jnp.float32
    )
    key_carried = jnp.einsum(
        "njv,ndv->njd", value_blk, state_grads, preferred_element_type=jnp.float32
    )
    value_carried = jnp.einsum(
        "njd,ndv->njv", key_dec, state_grads, preferred_element_type=jnp.float32
    )
    grad_q = query_inner + query_carried * query_scale[:, :, None]
    grad_k = key_inner + key_carried * key_scale[:, :, None]
    grad_v = value_inner + value_carried
    return (
        grad_q.reshape(length, key_width),
        grad_k.reshape(length, key_width),
        grad_v.reshape(length, value_width),
    )


def unit_grads(query_rows, key_rows, value_rows, grad_rows, decay_rows, backward):

    def orient(array):
        return jnp.where(backward, jnp.flip(array, 0), array)

    gradients = unit_backward(
        orient(query_rows),
        orient(key_rows),
        orient(value_rows),
        orient(grad_rows),
        orient(decay_rows),
        backward,
    )
    return tuple((orient(single).astype(jnp.bfloat16) for single in gradients))


def shards_by_unit(layer_input, queries, key_vectors, values, cotangent, log_decay, key_weight):
    tokens = layer_input.shape[1]
    key_width = queries.shape[2] // HEADS
    value_width = values.shape[2] // HEADS

    def to_units(array, head_width):
        shaped = array[0].reshape(tokens, HEADS, head_width)
        return jnp.moveaxis(jnp.repeat(shaped, 2, axis=1), 1, 0)

    sent = (
        to_units(queries, key_width),
        to_units(key_vectors, key_width),
        to_units(values, value_width),
        to_units(cotangent, value_width),
    )
    query_units, key_units, value_units, grad_units = (
        lax.all_to_all(sent[0], "sp", split_axis=0, concat_axis=1, tiled=True),
        lax.all_to_all(sent[1], "sp", split_axis=0, concat_axis=1, tiled=True),
        lax.all_to_all(sent[2], "sp", split_axis=0, concat_axis=1, tiled=True),
        lax.all_to_all(sent[3], "sp", split_axis=0, concat_axis=1, tiled=True),
    )
    local_units = query_units.shape[0]
    first_unit = lax.axis_index("sp") * local_units
    backward = (first_unit + jnp.arange(local_units)) % 2 == 1
    query_back, key_back, value_back = jax.vmap(unit_grads)(
        query_units, key_units, value_units, grad_units, log_decay[0], backward
    )
    query_home, key_home, value_home = (
        lax.all_to_all(query_back, "sp", split_axis=1, concat_axis=0, tiled=True),
        lax.all_to_all(key_back, "sp", split_axis=1, concat_axis=0, tiled=True),
        lax.all_to_all(value_back, "sp", split_axis=1, concat_axis=0, tiled=True),
    )

    def merge_dirs(array, head_width):
        paired = array.astype(jnp.float32).reshape(HEADS, 2, tokens, head_width).sum(axis=1)
        return jnp.moveaxis(paired, 0, 1).reshape(tokens, HEADS * head_width).astype(jnp.bfloat16)

    grad_query = merge_dirs(query_home, key_width)
    grad_key = merge_dirs(key_home, key_width)
    grad_value = merge_dirs(value_home, value_width)
    grad_input = lax.dot_general(
        grad_key,
        lax.all_gather(key_weight, "dp", axis=0, tiled=True),
        (((1,), (1,)), ((), ())),
        preferred_element_type=jnp.float32,
    ).astype(jnp.bfloat16)
    token_rows = layer_input[0]
    summed = lax.psum_scatter(
        lax.dot_general(
            token_rows, grad_key, (((0,), (0,)), ((), ())), preferred_element_type=jnp.float32
        ),
        "dp",
        scatter_dimension=0,
        tiled=True,
    )
    grad_weight = lax.psum(summed, "sp")
    return (grad_query[None], grad_value[None], grad_input[None], grad_weight)


def shards(*arrays):
    sp = lax.axis_size("sp")
    if sp == HEADS and arrays[1].shape[1] == BLOCK:
        return shards_by_head(sp, *arrays)
    return shards_by_unit(*arrays)


def solution(mesh):
    return jax.shard_map(
        shards,
        mesh=mesh,
        in_specs=(
            P("dp", "sp", None),
            P("dp", "sp", None),
            P("dp", "sp", None),
            P("dp", "sp", None),
            P("dp", "sp", None),
            P("dp", "sp", None),
            P("dp", None),
        ),
        out_specs=(P("dp", "sp", None), P("dp", "sp", None), P("dp", "sp", None), P("dp", None)),
        check_vma=False,
    )
```

```python
import functools

import jax
import jax.numpy as jnp
from jax import lax
from jax.experimental import pallas as pl
from jax.experimental.pallas import tpu as pltpu
from jax.sharding import PartitionSpec as P

HEADS = 8
BLOCK = 128
MESH = pl.DeviceIdType.MESH
BF16 = jnp.bfloat16
F32 = jnp.float32


def dot_nn(a, b):
    return lax.dot_general(a, b, (((1,), (0,)), ((), ())), preferred_element_type=F32)


def dot_nt(a, b):
    return lax.dot_general(a, b, (((1,), (1,)), ((), ())), preferred_element_type=F32)


def dot_tn(a, b):
    return lax.dot_general(a, b, (((0,), (0,)), ((), ())), preferred_element_type=F32)


def decay_columns(lam_ref, b):
    lam_fwd = lam_ref[0, b]
    lam_bwd = lam_ref[1, b]
    row = lax.broadcasted_iota(jnp.int32, (BLOCK, BLOCK), 0)
    col = lax.broadcasted_iota(jnp.int32, (BLOCK, BLOCK), 1)
    lower = col <= row
    c0 = jnp.sum(jnp.where(lower, lam_fwd, 0.0), axis=1, keepdims=True)
    c1 = jnp.sum(jnp.where(col >= row, lam_bwd, 0.0), axis=1, keepdims=True)
    e0 = jnp.sum(lam_fwd, axis=1, keepdims=True)
    e1 = jnp.sum(lam_bwd, axis=1, keepdims=True)
    return c0, c1, e0, e1, row, col, lower


def as_row(column, row, col):
    return jnp.sum(jnp.where(row == col, column, 0.0), axis=0, keepdims=True)


def retention_kernel(
    sp, dp,
    q_in, k_in, v_in, g_in, x_in, w_in, lam_ref,
    q_home, v_home, gi_out, dw_out,
    qa, ka, va, ga,
    qacc, kacc, vacc,
    dm0, dm1, dg0, dg1,
    sm0, sg1,
    run_a, run_b,
    qh, vh, kk, k_home, xa, wa, dw_send, dw_recv, dw_own, dw_sum,
    in_send, in_recv, x_send, x_recv, out_send, out_recv, local_sem,
    pair_send, pair_recv, w_send, w_recv, wf_send, wf_recv,
    rs_send, rs_recv, ag_send, ag_recv, x_sem, w_sem, ag_sem,
):
    me = lax.axis_index("sp")
    mine = lax.axis_index("dp")
    side = lax.rem(me, 2)
    partner = me + 1 - 2 * side
    sibling = mine + 1 - 2 * lax.rem(mine, 2)
    chips = dp // 2
    half = xa.shape[2]
    dk = qa.shape[1]
    dv = va.shape[1]
    scaling = dk ** (-0.5)
    ins = ((q_in, qa, dk), (k_in, ka, dk), (v_in, va, dv), (g_in, ga, dv))
    outs = ((qh, q_home, dk), (None, k_home, dk), (vh, v_home, dv))
    my_side = pl.ds(pl.multiple_of(side * dk, dk), dk)

    def rows_of(b):
        return pl.ds(pl.multiple_of(b * BLOCK, BLOCK), BLOCK)

    def cols_of(b, width):
        return pl.ds(pl.multiple_of(b * width, width), width)

    locals_in = [
        pltpu.make_async_copy(src.at[:, cols_of(me, w)], dst.at[rows_of(me)], local_sem.at[t])
        for t, (src, dst, w) in enumerate(ins)
    ]
    def x_cols(d, s):
        return pl.ds(pl.multiple_of((2 * d + s) * half, half), half)

    locals_x = [
        pltpu.make_async_copy(x_in.at[:, x_cols(d, side)], xa.at[d, rows_of(me)], x_sem.at[d])
        for d in range(dp)
    ]
    local_w = pltpu.make_async_copy(w_in, wa.at[mine], w_sem)
    for copy in locals_in:
        copy.start()

    barrier = pltpu.get_barrier_semaphore()
    for off in range(1, sp):
        pl.semaphore_signal(
            barrier, inc=1, device_id={"sp": lax.rem(me + off, sp)}, device_id_type=MESH
        )
    for off in range(1, dp):
        pl.semaphore_signal(
            barrier, inc=1, device_id={"dp": lax.rem(mine + off, dp)}, device_id_type=MESH
        )
    pl.semaphore_wait(barrier, sp + dp - 2)

    def incoming(t, off):
        src, dst, w = ins[t]
        peer = lax.rem(me + off, sp)
        return pltpu.make_async_remote_copy(
            src_ref=src.at[:, cols_of(peer, w)],
            dst_ref=dst.at[rows_of(me)],
            send_sem=in_send.at[t, off],
            recv_sem=in_recv.at[t, off],
            device_id={"sp": peer},
            device_id_type=MESH,
        )

    for off in range(1, sp):
        for t in range(4):
            incoming(t, off).start()

    def weight(off):
        return pltpu.make_async_remote_copy(
            src_ref=w_in, dst_ref=wa.at[mine],
            send_sem=w_send.at[off], recv_sem=w_recv.at[off],
            device_id={"dp": lax.rem(mine + 2 * off, dp)}, device_id_type=MESH,
        )

    def weight_across(off):
        owner = lax.rem(mine + dp - 2 * off, dp)
        return pltpu.make_async_remote_copy(
            src_ref=w_in if off == 0 else wa.at[owner], dst_ref=wa.at[owner],
            send_sem=wf_send.at[off], recv_sem=wf_recv.at[off],
            device_id={"dp": sibling}, device_id_type=MESH,
        )

    for off in range(1, chips):
        weight(off).start()
    weight_across(0).start()
    local_w.start()

    def rows_in(d, off):
        peer = lax.rem(me + off, sp)
        return pltpu.make_async_remote_copy(
            src_ref=x_in.at[:, x_cols(d, lax.rem(peer, 2))], dst_ref=xa.at[d, rows_of(me)],
            send_sem=x_send.at[d, off], recv_sem=x_recv.at[d, off],
            device_id={"sp": peer}, device_id_type=MESH,
        )

    for copy in locals_x:
        copy.start()
    for off in range(1, sp):
        for d in range(dp):
            rows_in(d, off).start()

    def local_part(b):
        rows = rows_of(b)
        q, k, v, g = qa[rows, :], ka[rows, :], va[rows, :], ga[rows, :]
        c0, c1, e0, e1, row, col, lower = decay_columns(lam_ref, b)
        spread = jnp.where(lower, c0 - as_row(c0, row, col), c1 - as_row(c1, row, col))
        weights = jnp.exp(spread) * scaling
        scores = (dot_nt(q, k) * weights).astype(BF16)
        grads = (dot_nt(g, v) * weights).astype(BF16)
        qacc[rows, :] = dot_nn(grads, k)
        kacc[rows, :] = dot_tn(grads, q)
        vacc[rows, :] = dot_tn(scores, g)
        qf, kf = q.astype(F32), k.astype(F32)
        dm0[b] = dot_tn((kf * jnp.exp(e0 - c0)).astype(BF16), v)
        dm1[b] = dot_tn((kf * jnp.exp(e1 - c1)).astype(BF16), v)
        dg0[b] = dot_tn((qf * (jnp.exp(c0) * scaling)).astype(BF16), g)
        dg1[b] = dot_tn((qf * (jnp.exp(c1) * scaling)).astype(BF16), g)

    for copy in locals_in:
        copy.wait()
    local_part(me)

    def arrive(off, carry):
        for t in range(4):
            incoming(t, off).wait_recv()
        local_part(lax.rem(me + sp - off, sp))
        return carry

    lax.fori_loop(1, sp, arrive, 0)

    run_a[...] = jnp.zeros_like(run_a)
    run_b[...] = jnp.zeros_like(run_b)

    def forward(b, carry):
        e0 = jnp.exp(jnp.sum(lam_ref[0, b], axis=1, keepdims=True))
        e1 = jnp.exp(jnp.sum(lam_ref[1, b], axis=1, keepdims=True))
        m0 = run_a[...]
        sm0[b] = m0.astype(BF16)
        run_a[...] = e0 * m0 + dm0[b]
        g1 = run_b[...]
        sg1[b] = g1.astype(BF16)
        run_b[...] = e1 * g1 + dg1[b]
        return carry

    lax.fori_loop(0, sp, forward, 0)

    for off in range(1, chips):
        weight(off).wait_recv()
        weight_across(off).start()

    run_a[...] = jnp.zeros_like(run_a)
    run_b[...] = jnp.zeros_like(run_b)

    def held(t, b):
        return kk.at[rows_of(b), my_side] if t == 1 else outs[t][0].at[rows_of(b)]

    def paired(b):
        return pltpu.make_async_remote_copy(
            src_ref=kk.at[rows_of(b), my_side], dst_ref=kk.at[rows_of(b), my_side],
            send_sem=pair_send.at[b], recv_sem=pair_recv.at[b],
            device_id={"sp": partner}, device_id_type=MESH,
        )

    def outgoing(t, b, source):
        _, dst, w = outs[t]
        return pltpu.make_async_remote_copy(
            src_ref=held(t, b),
            dst_ref=dst.at[:, cols_of(source, w)],
            send_sem=out_send.at[t, b],
            recv_sem=out_recv.at[t, source],
            device_id={"sp": b},
            device_id_type=MESH,
        )

    def local_out(t):
        _, dst, w = outs[t]
        return pltpu.make_async_copy(held(t, me), dst.at[:, cols_of(me, w)], local_sem.at[t])

    def backward(step, carry):
        b = sp - 1 - step
        rows = rows_of(b)
        k, v, g = ka[rows, :], va[rows, :], ga[rows, :]
        c0, c1, e0, e1, _, _, _ = decay_columns(lam_ref, b)
        kf = k.astype(F32)
        ks0, ks1 = jnp.exp(e0 - c0), jnp.exp(e1 - c1)
        m0, g1 = sm0[b], sg1[b]
        g0, m1 = run_a[...].astype(BF16), run_b[...].astype(BF16)
        qh[rows, :] = (
            qacc[rows, :]
            + dot_nt(g, m0) * (jnp.exp(c0) * scaling)
            + dot_nt(g, m1) * (jnp.exp(c1) * scaling)
        ).astype(BF16)
        kk[rows, my_side] = (
            kacc[rows, :] + dot_nt(v, g0) * ks0 + dot_nt(v, g1) * ks1
        ).astype(BF16)
        vh[rows, :] = (
            vacc[rows, :]
            + dot_nn((kf * ks0).astype(BF16), g0)
            + dot_nn((kf * ks1).astype(BF16), g1)
        ).astype(BF16)
        run_a[...] = jnp.exp(e0) * run_a[...] + dg0[b]
        run_b[...] = jnp.exp(e1) * run_b[...] + dm1[b]

        paired(b).start()

        @pl.when(b != me)
        def _():
            for t in (1, 0, 2):
                outgoing(t, b, me).start()

        @pl.when(b == me)
        def _():
            for t in range(3):
                local_out(t).start()

        return carry

    lax.fori_loop(0, sp, backward, 0)

    for copy in locals_x:
        copy.wait()

    def rows_arrived(off, carry):
        for d in range(dp):
            rows_in(d, off).wait_recv()
        return carry

    lax.fori_loop(1, sp, rows_arrived, 0)

    def pair_arrived(b, carry):
        paired(b).wait()
        return carry

    lax.fori_loop(0, sp, pair_arrived, 0)

    def reducing(off):
        peer = lax.rem(mine + off, dp)
        return pltpu.make_async_remote_copy(
            src_ref=dw_send.at[off], dst_ref=dw_recv.at[off],
            send_sem=rs_send.at[off], recv_sem=rs_recv.at[off],
            device_id={"dp": peer}, device_id_type=MESH,
        )

    for off in range(1, dp):
        dw_send[off] = dot_tn(xa[lax.rem(mine + off, dp)], kk[...]).astype(BF16)
    for off in range(1, dp):
        reducing(off).start()
    dw_own[...] = dot_tn(xa[mine], kk[...])
    for off in range(1, dp):
        reducing(off).wait_recv()
        dw_own[...] += dw_recv[off].astype(F32)
    dw_sum[...] = dw_own[...].astype(BF16)

    def spot(device):
        s = lax.rem(device, 2)
        z = device // 2
        return (
            pl.ds(pl.multiple_of(s * half, half), half),
            pl.ds(pl.multiple_of(z * (2 * dk), 2 * dk), 2 * dk),
        )

    def spreading(off):
        return pltpu.make_async_remote_copy(
            src_ref=dw_sum, dst_ref=dw_out.at[spot(me)],
            send_sem=ag_send.at[off], recv_sem=ag_recv.at[off],
            device_id={"sp": lax.rem(me + off, sp)}, device_id_type=MESH,
        )

    own_spot = pltpu.make_async_copy(dw_sum, dw_out.at[spot(me)], ag_sem)
    own_spot.start()
    for off in range(1, sp):
        spreading(off).start()

    for t in range(3):
        local_out(t).wait()

    def settle(off, carry):
        peer = lax.rem(me + off, sp)
        for t in range(3):
            outgoing(t, peer, peer).wait()
        return carry

    lax.fori_loop(1, sp, settle, 0)
    local_w.wait()
    for off in range(chips):
        weight_across(off).wait()
    rows_each = wa.shape[1]
    for d in range(dp):
        gi_out[:, d * rows_each : (d + 1) * rows_each] = dot_nt(k_home[...], wa[d]).astype(BF16)

    for off in range(1, chips):
        weight(off).wait_send()
    for off in range(1, sp):
        for t in range(4):
            incoming(t, off).wait_send()
        for d in range(dp):
            rows_in(d, off).wait_send()
    for off in range(1, dp):
        reducing(off).wait_send()
    own_spot.wait()
    for off in range(1, sp):
        spreading(off).wait()


def shards_by_head(sp, dp, layer_input, queries, key_vectors, values, cotangent, log_decay, key_weight):
    _, tokens, hk = queries.shape
    hv = values.shape[2]
    rows, width = key_weight.shape
    length = tokens * sp
    dk, dv = hk // HEADS, hv // HEADS
    half = rows // 2
    lam = log_decay.reshape(2, sp, 1, BLOCK)
    anyspace = pl.BlockSpec(memory_space=pl.ANY)
    vmem = pl.BlockSpec(memory_space=pltpu.VMEM)
    dma = pltpu.SemaphoreType.DMA
    grad_query, grad_value, grad_input, grad_weight = pl.pallas_call(
        functools.partial(retention_kernel, sp, dp),
        out_shape=(
            jax.ShapeDtypeStruct((tokens, hk), BF16),
            jax.ShapeDtypeStruct((tokens, hv), BF16),
            jax.ShapeDtypeStruct((tokens, rows * dp), BF16),
            jax.ShapeDtypeStruct((rows, hk), BF16),
        ),
        in_specs=[anyspace] * 6 + [vmem],
        out_specs=(anyspace, anyspace, vmem, anyspace),
        scratch_shapes=[
            pltpu.VMEM((length, dk), BF16),
            pltpu.VMEM((length, dk), BF16),
            pltpu.VMEM((length, dv), BF16),
            pltpu.VMEM((length, dv), BF16),
            pltpu.VMEM((length, dk), F32),
            pltpu.VMEM((length, dk), F32),
            pltpu.VMEM((length, dv), F32),
            pltpu.VMEM((sp, dk, dv), F32),
            pltpu.VMEM((sp, dk, dv), F32),
            pltpu.VMEM((sp, dk, dv), F32),
            pltpu.VMEM((sp, dk, dv), F32),
            pltpu.VMEM((sp, dk, dv), BF16),
            pltpu.VMEM((sp, dk, dv), BF16),
            pltpu.VMEM((dk, dv), F32),
            pltpu.VMEM((dk, dv), F32),
            pltpu.VMEM((length, dk), BF16),
            pltpu.VMEM((length, dv), BF16),
            pltpu.VMEM((length, 2 * dk), BF16),
            pltpu.VMEM((tokens, hk), BF16),
            pltpu.VMEM((dp, length, half), BF16),
            pltpu.VMEM((dp, rows, width), BF16),
            pltpu.VMEM((dp, half, 2 * dk), BF16),
            pltpu.VMEM((dp, half, 2 * dk), BF16),
            pltpu.VMEM((half, 2 * dk), F32),
            pltpu.VMEM((half, 2 * dk), BF16),
            dma((4, sp)), dma((4, sp)), dma((dp, sp)), dma((dp, sp)),
            dma((3, sp)), dma((3, sp)), dma((4,)),
            dma((sp,)), dma((sp,)), dma((dp,)), dma((dp,)), dma((dp,)), dma((dp,)),
            dma((dp,)), dma((dp,)), dma((sp,)), dma((sp,)), dma((dp,)), dma(()), dma(()),
        ],
        compiler_params=pltpu.CompilerParams(
            collective_id=0, has_side_effects=True, vmem_limit_bytes=60 * 1024 * 1024
        ),
    )(queries[0], key_vectors[0], values[0], cotangent[0], layer_input[0], key_weight, lam)
    return (grad_query[None], grad_value[None], grad_input[None], grad_weight.astype(F32))


def unit_backward(query_rows, key_rows, value_rows, grad_rows, decay_rows, strict):
    length, key_width = query_rows.shape
    value_width = value_rows.shape[1]
    blocks = length // BLOCK
    scaling = key_width ** (-0.5)
    query_blk = query_rows.reshape(blocks, BLOCK, key_width)
    key_blk = key_rows.reshape(blocks, BLOCK, key_width)
    value_blk = value_rows.reshape(blocks, BLOCK, value_width)
    grad_blk = grad_rows.reshape(blocks, BLOCK, value_width)
    within = jnp.cumsum(decay_rows.reshape(blocks, BLOCK), axis=1)
    position_slots = jnp.arange(BLOCK)
    allowed = jnp.where(
        strict,
        position_slots[None, :] < position_slots[:, None],
        position_slots[None, :] <= position_slots[:, None],
    )
    spread = jnp.where(allowed, within[:, :, None] - within[:, None, :], 0.0)
    weights = jnp.where(allowed, jnp.exp(spread), 0.0) * scaling
    raw_scores = jnp.einsum("nid,njd->nij", query_blk, key_blk, preferred_element_type=jnp.float32)
    scores = (raw_scores * weights).astype(jnp.bfloat16)
    raw_grads = jnp.einsum("niv,njv->nij", grad_blk, value_blk, preferred_element_type=jnp.float32)
    grad_scores = (raw_grads * weights).astype(jnp.bfloat16)
    value_inner = jnp.einsum("nij,niv->njv", scores, grad_blk, preferred_element_type=jnp.float32)
    query_inner = jnp.einsum(
        "nij,njd->nid", grad_scores, key_blk, preferred_element_type=jnp.float32
    )
    key_inner = jnp.einsum(
        "nij,nid->njd", grad_scores, query_blk, preferred_element_type=jnp.float32
    )
    ending = within[:, -1:]
    query_scale = jnp.exp(within) * scaling
    key_scale = jnp.exp(ending - within)
    carry_decay = jnp.exp(ending[:, 0])
    query_dec = (query_blk * query_scale[:, :, None]).astype(jnp.bfloat16)
    key_dec = (key_blk * key_scale[:, :, None]).astype(jnp.bfloat16)
    contract = (((0,), (0,)), ((), ()))

    def advance(memory, inputs):
        key_b, value_b, factor = inputs
        before = memory.astype(jnp.bfloat16)
        memory = factor * memory + lax.dot_general(
            key_b, value_b, contract, preferred_element_type=jnp.float32
        )
        return (memory, before)

    start_state = jnp.zeros((key_width, value_width), jnp.float32)
    _, states_before = lax.scan(advance, start_state, (key_dec, value_blk, carry_decay))

    def retreat(later, inputs):
        query_b, grad_b, factor = inputs
        after = later.astype(jnp.bfloat16)
        later = factor * later + lax.dot_general(
            query_b, grad_b, contract, preferred_element_type=jnp.float32
        )
        return (later, after)

    _, state_grads = lax.scan(
        retreat, start_state, (query_dec, grad_blk, carry_decay), reverse=True
    )
    query_carried = jnp.einsum(
        "niv,ndv->nid", grad_blk, states_before, preferred_element_type=jnp.float32
    )
    key_carried = jnp.einsum(
        "njv,ndv->njd", value_blk, state_grads, preferred_element_type=jnp.float32
    )
    value_carried = jnp.einsum(
        "njd,ndv->njv", key_dec, state_grads, preferred_element_type=jnp.float32
    )
    grad_q = query_inner + query_carried * query_scale[:, :, None]
    grad_k = key_inner + key_carried * key_scale[:, :, None]
    grad_v = value_inner + value_carried
    return (
        grad_q.reshape(length, key_width),
        grad_k.reshape(length, key_width),
        grad_v.reshape(length, value_width),
    )


def unit_grads(query_rows, key_rows, value_rows, grad_rows, decay_rows, backward):

    def orient(array):
        return jnp.where(backward, jnp.flip(array, 0), array)

    gradients = unit_backward(
        orient(query_rows),
        orient(key_rows),
        orient(value_rows),
        orient(grad_rows),
        orient(decay_rows),
        backward,
    )
    return tuple((orient(single).astype(jnp.bfloat16) for single in gradients))


def shards_by_unit(layer_input, queries, key_vectors, values, cotangent, log_decay, key_weight):
    tokens = layer_input.shape[1]
    key_width = queries.shape[2] // HEADS
    value_width = values.shape[2] // HEADS

    def to_units(array, head_width):
        shaped = array[0].reshape(tokens, HEADS, head_width)
        return jnp.moveaxis(jnp.repeat(shaped, 2, axis=1), 1, 0)

    sent = (
        to_units(queries, key_width),
        to_units(key_vectors, key_width),
        to_units(values, value_width),
        to_units(cotangent, value_width),
    )
    query_units, key_units, value_units, grad_units = (
        lax.all_to_all(sent[0], "sp", split_axis=0, concat_axis=1, tiled=True),
        lax.all_to_all(sent[1], "sp", split_axis=0, concat_axis=1, tiled=True),
        lax.all_to_all(sent[2], "sp", split_axis=0, concat_axis=1, tiled=True),
        lax.all_to_all(sent[3], "sp", split_axis=0, concat_axis=1, tiled=True),
    )
    local_units = query_units.shape[0]
    first_unit = lax.axis_index("sp") * local_units
    backward = (first_unit + jnp.arange(local_units)) % 2 == 1
    query_back, key_back, value_back = jax.vmap(unit_grads)(
        query_units, key_units, value_units, grad_units, log_decay[0], backward
    )
    query_home, key_home, value_home = (
        lax.all_to_all(query_back, "sp", split_axis=1, concat_axis=0, tiled=True),
        lax.all_to_all(key_back, "sp", split_axis=1, concat_axis=0, tiled=True),
        lax.all_to_all(value_back, "sp", split_axis=1, concat_axis=0, tiled=True),
    )

    def merge_dirs(array, head_width):
        paired = array.astype(jnp.float32).reshape(HEADS, 2, tokens, head_width).sum(axis=1)
        return jnp.moveaxis(paired, 0, 1).reshape(tokens, HEADS * head_width).astype(jnp.bfloat16)

    grad_query = merge_dirs(query_home, key_width)
    grad_key = merge_dirs(key_home, key_width)
    grad_value = merge_dirs(value_home, value_width)
    grad_input = lax.dot_general(
        grad_key,
        lax.all_gather(key_weight, "dp", axis=0, tiled=True),
        (((1,), (1,)), ((), ())),
        preferred_element_type=jnp.float32,
    ).astype(jnp.bfloat16)
    token_rows = layer_input[0]
    summed = lax.psum_scatter(
        lax.dot_general(
            token_rows, grad_key, (((0,), (0,)), ((), ())), preferred_element_type=jnp.float32
        ),
        "dp",
        scatter_dimension=0,
        tiled=True,
    )
    grad_weight = lax.psum(summed, "sp")
    return (grad_query[None], grad_value[None], grad_input[None], grad_weight)


def shards(*arrays):
    sp = lax.axis_size("sp")
    dp = lax.axis_size("dp")
    if sp == HEADS and arrays[1].shape[1] == BLOCK and dp % 2 == 0:
        return shards_by_head(sp, dp, *arrays)
    return shards_by_unit(*arrays)


def solution(mesh):
    return jax.shard_map(
        shards,
        mesh=mesh,
        in_specs=(
            P("dp", "sp", None),
            P("dp", "sp", None),
            P("dp", "sp", None),
            P("dp", "sp", None),
            P("dp", "sp", None),
            P("dp", "sp", None),
            P("dp", None),
        ),
        out_specs=(P("dp", "sp", None), P("dp", "sp", None), P("dp", "sp", None), P("dp", None)),
        check_vma=False,
    )
```

```python
import functools

import jax
import jax.numpy as jnp
from jax import lax
from jax.experimental import pallas as pl
from jax.experimental.pallas import tpu as pltpu
from jax.sharding import PartitionSpec as P

HEADS = 8
BLOCK = 128
MESH = pl.DeviceIdType.MESH
BF16 = jnp.bfloat16
F32 = jnp.float32


def dot_nn(a, b):
    return lax.dot_general(a, b, (((1,), (0,)), ((), ())), preferred_element_type=F32)


def dot_nt(a, b):
    return lax.dot_general(a, b, (((1,), (1,)), ((), ())), preferred_element_type=F32)


def dot_tn(a, b):
    return lax.dot_general(a, b, (((0,), (0,)), ((), ())), preferred_element_type=F32)


def decay_columns(lam_ref, b):
    lam_fwd = lam_ref[0, b]
    lam_bwd = lam_ref[1, b]
    row = lax.broadcasted_iota(jnp.int32, (BLOCK, BLOCK), 0)
    col = lax.broadcasted_iota(jnp.int32, (BLOCK, BLOCK), 1)
    lower = col <= row
    c0 = jnp.sum(jnp.where(lower, lam_fwd, 0.0), axis=1, keepdims=True)
    c1 = jnp.sum(jnp.where(col >= row, lam_bwd, 0.0), axis=1, keepdims=True)
    e0 = jnp.sum(lam_fwd, axis=1, keepdims=True)
    e1 = jnp.sum(lam_bwd, axis=1, keepdims=True)
    return c0, c1, e0, e1, row, col, lower


def as_row(column, row, col):
    return jnp.sum(jnp.where(row == col, column, 0.0), axis=0, keepdims=True)


def retention_kernel(
    sp, dp,
    q_in, k_in, v_in, g_in, x_in, w_in, lam_ref,
    q_home, v_home, gi_out, dw_out,
    qa, ka, va, ga,
    qacc, kacc, vacc,
    dm0, dm1, dg0, dg1,
    sm0, sg1,
    run_a, run_b,
    qh, vh, kk, k_home, xa, wa, dw_send, dw_recv, dw_own, dw_sum,
    in_send, in_recv, x_send, x_recv, out_send, out_recv, local_sem,
    pair_send, pair_recv, w_send, w_recv, wf_send, wf_recv,
    rs_send, rs_recv, ag_send, ag_recv, x_sem, w_sem, ag_sem,
    xf, xc_send, xc_recv, xg_send, xg_recv, af_send, af_recv,
):
    me = lax.axis_index("sp")
    mine = lax.axis_index("dp")
    side = lax.rem(me, 2)
    partner = me + 1 - 2 * side
    sibling = mine + 1 - 2 * lax.rem(mine, 2)
    chips = dp // 2
    group = sp // 2
    first = (me // group) * group
    far = lax.rem(me + group, sp)

    def near(off):
        return first + lax.rem(me - first + off, group)

    half = xa.shape[2]
    dk = qa.shape[1]
    dv = va.shape[1]
    scaling = dk ** (-0.5)
    ins = ((q_in, qa, dk), (k_in, ka, dk), (v_in, va, dv), (g_in, ga, dv))
    outs = ((qh, q_home, dk), (None, k_home, dk), (vh, v_home, dv))
    my_side = pl.ds(pl.multiple_of(side * dk, dk), dk)

    def rows_of(b):
        return pl.ds(pl.multiple_of(b * BLOCK, BLOCK), BLOCK)

    def cols_of(b, width):
        return pl.ds(pl.multiple_of(b * width, width), width)

    locals_in = [
        pltpu.make_async_copy(src.at[:, cols_of(me, w)], dst.at[rows_of(me)], local_sem.at[t])
        for t, (src, dst, w) in enumerate(ins)
    ]
    def x_cols(d, s):
        return pl.ds(pl.multiple_of((2 * d + s) * half, half), half)

    locals_x = [
        pltpu.make_async_copy(x_in.at[:, x_cols(d, side)], xa.at[d, rows_of(me)], x_sem.at[d])
        for d in range(dp)
    ]
    local_w = pltpu.make_async_copy(w_in, wa.at[mine], w_sem)
    for copy in locals_in:
        copy.start()

    barrier = pltpu.get_barrier_semaphore()
    for off in range(1, sp):
        pl.semaphore_signal(
            barrier, inc=1, device_id={"sp": lax.rem(me + off, sp)}, device_id_type=MESH
        )
    for off in range(1, dp):
        pl.semaphore_signal(
            barrier, inc=1, device_id={"dp": lax.rem(mine + off, dp)}, device_id_type=MESH
        )
    pl.semaphore_wait(barrier, sp + dp - 2)

    def incoming(t, off):
        src, dst, w = ins[t]
        peer = lax.rem(me + off, sp)
        return pltpu.make_async_remote_copy(
            src_ref=src.at[:, cols_of(peer, w)],
            dst_ref=dst.at[rows_of(me)],
            send_sem=in_send.at[t, off],
            recv_sem=in_recv.at[t, off],
            device_id={"sp": peer},
            device_id_type=MESH,
        )

    for off in range(1, sp):
        for t in range(4):
            incoming(t, off).start()

    def weight(off):
        return pltpu.make_async_remote_copy(
            src_ref=w_in, dst_ref=wa.at[mine],
            send_sem=w_send.at[off], recv_sem=w_recv.at[off],
            device_id={"dp": lax.rem(mine + 2 * off, dp)}, device_id_type=MESH,
        )

    def weight_across(off):
        owner = lax.rem(mine + dp - 2 * off, dp)
        return pltpu.make_async_remote_copy(
            src_ref=w_in if off == 0 else wa.at[owner], dst_ref=wa.at[owner],
            send_sem=wf_send.at[off], recv_sem=wf_recv.at[off],
            device_id={"dp": sibling}, device_id_type=MESH,
        )

    for off in range(1, chips):
        weight(off).start()
    weight_across(0).start()
    local_w.start()

    def rows_in(d, off):
        peer = near(off) if off else far
        return pltpu.make_async_remote_copy(
            src_ref=x_in.at[:, x_cols(d, lax.rem(peer, 2))], dst_ref=xa.at[d, rows_of(me)],
            send_sem=x_send.at[d, off], recv_sem=x_recv.at[d, off],
            device_id={"sp": peer}, device_id_type=MESH,
        )

    def rows_far(d):
        return pltpu.make_async_remote_copy(
            src_ref=x_in.at[:, x_cols(d, 1 - side)], dst_ref=xf.at[d],
            send_sem=xc_send.at[d], recv_sem=xc_recv.at[d],
            device_id={"sp": far}, device_id_type=MESH,
        )

    def rows_on(d, off):
        return pltpu.make_async_remote_copy(
            src_ref=xa.at[d, rows_of(far)] if off % 2 == 0 else xf.at[d],
            dst_ref=xa.at[d, rows_of(far)],
            send_sem=xg_send.at[d, off], recv_sem=xg_recv.at[d, off],
            device_id={"sp": near(off)}, device_id_type=MESH,
        )

    for copy in locals_x:
        copy.start()
    for d in range(dp):
        rows_in(d, 0).start()
        rows_far(d).start()
    for off in range(1, group):
        for d in range(dp):
            rows_in(d, off).start()

    def local_part(b):
        rows = rows_of(b)
        q, k, v, g = qa[rows, :], ka[rows, :], va[rows, :], ga[rows, :]
        c0, c1, e0, e1, row, col, lower = decay_columns(lam_ref, b)
        spread = jnp.where(lower, c0 - as_row(c0, row, col), c1 - as_row(c1, row, col))
        weights = jnp.exp(spread) * scaling
        scores = (dot_nt(q, k) * weights).astype(BF16)
        grads = (dot_nt(g, v) * weights).astype(BF16)
        qacc[rows, :] = dot_nn(grads, k)
        kacc[rows, :] = dot_tn(grads, q)
        vacc[rows, :] = dot_tn(scores, g)
        qf, kf = q.astype(F32), k.astype(F32)
        dm0[b] = dot_tn((kf * jnp.exp(e0 - c0)).astype(BF16), v)
        dm1[b] = dot_tn((kf * jnp.exp(e1 - c1)).astype(BF16), v)
        dg0[b] = dot_tn((qf * (jnp.exp(c0) * scaling)).astype(BF16), g)
        dg1[b] = dot_tn((qf * (jnp.exp(c1) * scaling)).astype(BF16), g)

    for copy in locals_in:
        copy.wait()
    local_part(me)

    def arrive(off, carry):
        for t in range(4):
            incoming(t, off).wait_recv()
        local_part(lax.rem(me + sp - off, sp))
        return carry

    lax.fori_loop(1, sp, arrive, 0)

    run_a[...] = jnp.zeros_like(run_a)
    run_b[...] = jnp.zeros_like(run_b)

    def forward(b, carry):
        e0 = jnp.exp(jnp.sum(lam_ref[0, b], axis=1, keepdims=True))
        e1 = jnp.exp(jnp.sum(lam_ref[1, b], axis=1, keepdims=True))
        m0 = run_a[...]
        sm0[b] = m0.astype(BF16)
        run_a[...] = e0 * m0 + dm0[b]
        g1 = run_b[...]
        sg1[b] = g1.astype(BF16)
        run_b[...] = e1 * g1 + dg1[b]
        return carry

    lax.fori_loop(0, sp, forward, 0)

    for off in range(1, chips):
        weight(off).wait_recv()
        weight_across(off).start()

    run_a[...] = jnp.zeros_like(run_a)
    run_b[...] = jnp.zeros_like(run_b)

    def held(t, b):
        return kk.at[rows_of(b), my_side] if t == 1 else outs[t][0].at[rows_of(b)]

    def paired(b):
        return pltpu.make_async_remote_copy(
            src_ref=kk.at[rows_of(b), my_side], dst_ref=kk.at[rows_of(b), my_side],
            send_sem=pair_send.at[b], recv_sem=pair_recv.at[b],
            device_id={"sp": partner}, device_id_type=MESH,
        )

    def outgoing(t, b, source):
        _, dst, w = outs[t]
        return pltpu.make_async_remote_copy(
            src_ref=held(t, b),
            dst_ref=dst.at[:, cols_of(source, w)],
            send_sem=out_send.at[t, b],
            recv_sem=out_recv.at[t, source],
            device_id={"sp": b},
            device_id_type=MESH,
        )

    def local_out(t):
        _, dst, w = outs[t]
        return pltpu.make_async_copy(held(t, me), dst.at[:, cols_of(me, w)], local_sem.at[t])

    def backward(step, carry):
        b = sp - 1 - step
        rows = rows_of(b)
        k, v, g = ka[rows, :], va[rows, :], ga[rows, :]
        c0, c1, e0, e1, _, _, _ = decay_columns(lam_ref, b)
        kf = k.astype(F32)
        ks0, ks1 = jnp.exp(e0 - c0), jnp.exp(e1 - c1)
        m0, g1 = sm0[b], sg1[b]
        g0, m1 = run_a[...].astype(BF16), run_b[...].astype(BF16)
        qh[rows, :] = (
            qacc[rows, :]
            + dot_nt(g, m0) * (jnp.exp(c0) * scaling)
            + dot_nt(g, m1) * (jnp.exp(c1) * scaling)
        ).astype(BF16)
        kk[rows, my_side] = (
            kacc[rows, :] + dot_nt(v, g0) * ks0 + dot_nt(v, g1) * ks1
        ).astype(BF16)
        vh[rows, :] = (
            vacc[rows, :]
            + dot_nn((kf * ks0).astype(BF16), g0)
            + dot_nn((kf * ks1).astype(BF16), g1)
        ).astype(BF16)
        run_a[...] = jnp.exp(e0) * run_a[...] + dg0[b]
        run_b[...] = jnp.exp(e1) * run_b[...] + dm1[b]

        paired(b).start()

        @pl.when(b != me)
        def _():
            outgoing(1, b, me).start()

        @pl.when(b == me)
        def _():
            local_out(1).start()

        return carry

    lax.fori_loop(0, sp, backward, 0)

    for copy in locals_x:
        copy.wait()

    for d in range(dp):
        rows_in(d, 0).wait_recv()
        rows_far(d).wait_recv()
    for off in range(1, group):
        for d in range(dp):
            rows_on(d, off).start()

    for t in (0, 2):
        local_out(t).start()

    def send_rest(step, carry):
        b = lax.rem(far + step, sp)
        for t in (0, 2):
            outgoing(t, b, me).start()
        return carry

    lax.fori_loop(0, group, send_rest, 0)
    lax.fori_loop(group + 1, sp, send_rest, 0)

    for off in range(1, group):
        for d in range(dp):
            rows_in(d, off).wait_recv()
    for off in range(1, group):
        for d in range(dp):
            rows_on(d, off).wait_recv()

    def pair_arrived(b, carry):
        paired(b).wait()
        return carry

    lax.fori_loop(0, sp, pair_arrived, 0)

    def reducing(off):
        peer = lax.rem(mine + off, dp)
        return pltpu.make_async_remote_copy(
            src_ref=dw_send.at[off], dst_ref=dw_recv.at[off],
            send_sem=rs_send.at[off], recv_sem=rs_recv.at[off],
            device_id={"dp": peer}, device_id_type=MESH,
        )

    for off in range(1, dp):
        dw_send[off] = dot_tn(xa[lax.rem(mine + off, dp)], kk[...]).astype(BF16)
    for off in range(1, dp):
        reducing(off).start()
    dw_own[...] = dot_tn(xa[mine], kk[...])
    for off in range(1, dp):
        reducing(off).wait_recv()
        dw_own[...] += dw_recv[off].astype(F32)
    dw_sum[...] = dw_own[...].astype(BF16)

    def spot(device):
        s = lax.rem(device, 2)
        z = device // 2
        return (
            pl.ds(pl.multiple_of(s * half, half), half),
            pl.ds(pl.multiple_of(z * (2 * dk), 2 * dk), 2 * dk),
        )

    def spreading(off):
        return pltpu.make_async_remote_copy(
            src_ref=dw_sum, dst_ref=dw_out.at[spot(me)],
            send_sem=ag_send.at[off], recv_sem=ag_recv.at[off],
            device_id={"sp": near(off) if off else far}, device_id_type=MESH,
        )

    def passing(off):
        return pltpu.make_async_remote_copy(
            src_ref=dw_out.at[spot(far)], dst_ref=dw_out.at[spot(far)],
            send_sem=af_send.at[off], recv_sem=af_recv.at[off],
            device_id={"sp": near(off)}, device_id_type=MESH,
        )

    own_spot = pltpu.make_async_copy(dw_sum, dw_out.at[spot(me)], ag_sem)
    own_spot.start()
    for off in range(group):
        spreading(off).start()
    spreading(0).wait_recv()
    for off in range(1, group):
        passing(off).start()

    for t in range(3):
        local_out(t).wait()

    def settle(off, carry):
        peer = lax.rem(me + off, sp)
        for t in range(3):
            outgoing(t, peer, peer).wait()
        return carry

    lax.fori_loop(1, sp, settle, 0)
    local_w.wait()
    for off in range(chips):
        weight_across(off).wait()
    rows_each = wa.shape[1]
    for d in range(dp):
        gi_out[:, d * rows_each : (d + 1) * rows_each] = dot_nt(k_home[...], wa[d]).astype(BF16)

    for off in range(1, chips):
        weight(off).wait_send()
    for off in range(1, sp):
        for t in range(4):
            incoming(t, off).wait_send()
    for d in range(dp):
        rows_far(d).wait_send()
        for off in range(group):
            rows_in(d, off).wait_send()
        for off in range(1, group):
            rows_on(d, off).wait_send()
    for off in range(1, dp):
        reducing(off).wait_send()
    own_spot.wait()
    spreading(0).wait_send()
    for off in range(1, group):
        spreading(off).wait()
        passing(off).wait()


def shards_by_head(sp, dp, layer_input, queries, key_vectors, values, cotangent, log_decay, key_weight):
    _, tokens, hk = queries.shape
    hv = values.shape[2]
    rows, width = key_weight.shape
    length = tokens * sp
    dk, dv = hk // HEADS, hv // HEADS
    half = rows // 2
    lam = log_decay.reshape(2, sp, 1, BLOCK)
    anyspace = pl.BlockSpec(memory_space=pl.ANY)
    vmem = pl.BlockSpec(memory_space=pltpu.VMEM)
    dma = pltpu.SemaphoreType.DMA
    grad_query, grad_value, grad_input, grad_weight = pl.pallas_call(
        functools.partial(retention_kernel, sp, dp),
        out_shape=(
            jax.ShapeDtypeStruct((tokens, hk), BF16),
            jax.ShapeDtypeStruct((tokens, hv), BF16),
            jax.ShapeDtypeStruct((tokens, rows * dp), BF16),
            jax.ShapeDtypeStruct((rows, hk), BF16),
        ),
        in_specs=[anyspace] * 6 + [vmem],
        out_specs=(anyspace, anyspace, vmem, anyspace),
        scratch_shapes=[
            pltpu.VMEM((length, dk), BF16),
            pltpu.VMEM((length, dk), BF16),
            pltpu.VMEM((length, dv), BF16),
            pltpu.VMEM((length, dv), BF16),
            pltpu.VMEM((length, dk), F32),
            pltpu.VMEM((length, dk), F32),
            pltpu.VMEM((length, dv), F32),
            pltpu.VMEM((sp, dk, dv), F32),
            pltpu.VMEM((sp, dk, dv), F32),
            pltpu.VMEM((sp, dk, dv), F32),
            pltpu.VMEM((sp, dk, dv), F32),
            pltpu.VMEM((sp, dk, dv), BF16),
            pltpu.VMEM((sp, dk, dv), BF16),
            pltpu.VMEM((dk, dv), F32),
            pltpu.VMEM((dk, dv), F32),
            pltpu.VMEM((length, dk), BF16),
            pltpu.VMEM((length, dv), BF16),
            pltpu.VMEM((length, 2 * dk), BF16),
            pltpu.VMEM((tokens, hk), BF16),
            pltpu.VMEM((dp, length, half), BF16),
            pltpu.VMEM((dp, rows, width), BF16),
            pltpu.VMEM((dp, half, 2 * dk), BF16),
            pltpu.VMEM((dp, half, 2 * dk), BF16),
            pltpu.VMEM((half, 2 * dk), F32),
            pltpu.VMEM((half, 2 * dk), BF16),
            dma((4, sp)), dma((4, sp)), dma((dp, sp)), dma((dp, sp)),
            dma((3, sp)), dma((3, sp)), dma((4,)),
            dma((sp,)), dma((sp,)), dma((dp,)), dma((dp,)), dma((dp,)), dma((dp,)),
            dma((dp,)), dma((dp,)), dma((sp,)), dma((sp,)), dma((dp,)), dma(()), dma(()),
            pltpu.VMEM((dp, tokens, half), BF16),
            dma((dp,)), dma((dp,)), dma((dp, sp)), dma((dp, sp)), dma((sp,)), dma((sp,)),
        ],
        compiler_params=pltpu.CompilerParams(
            collective_id=0, has_side_effects=True, vmem_limit_bytes=60 * 1024 * 1024
        ),
    )(queries[0], key_vectors[0], values[0], cotangent[0], layer_input[0], key_weight, lam)
    return (grad_query[None], grad_value[None], grad_input[None], grad_weight.astype(F32))


def unit_backward(query_rows, key_rows, value_rows, grad_rows, decay_rows, strict):
    length, key_width = query_rows.shape
    value_width = value_rows.shape[1]
    blocks = length // BLOCK
    scaling = key_width ** (-0.5)
    query_blk = query_rows.reshape(blocks, BLOCK, key_width)
    key_blk = key_rows.reshape(blocks, BLOCK, key_width)
    value_blk = value_rows.reshape(blocks, BLOCK, value_width)
    grad_blk = grad_rows.reshape(blocks, BLOCK, value_width)
    within = jnp.cumsum(decay_rows.reshape(blocks, BLOCK), axis=1)
    position_slots = jnp.arange(BLOCK)
    allowed = jnp.where(
        strict,
        position_slots[None, :] < position_slots[:, None],
        position_slots[None, :] <= position_slots[:, None],
    )
    spread = jnp.where(allowed, within[:, :, None] - within[:, None, :], 0.0)
    weights = jnp.where(allowed, jnp.exp(spread), 0.0) * scaling
    raw_scores = jnp.einsum("nid,njd->nij", query_blk, key_blk, preferred_element_type=jnp.float32)
    scores = (raw_scores * weights).astype(jnp.bfloat16)
    raw_grads = jnp.einsum("niv,njv->nij", grad_blk, value_blk, preferred_element_type=jnp.float32)
    grad_scores = (raw_grads * weights).astype(jnp.bfloat16)
    value_inner = jnp.einsum("nij,niv->njv", scores, grad_blk, preferred_element_type=jnp.float32)
    query_inner = jnp.einsum(
        "nij,njd->nid", grad_scores, key_blk, preferred_element_type=jnp.float32
    )
    key_inner = jnp.einsum(
        "nij,nid->njd", grad_scores, query_blk, preferred_element_type=jnp.float32
    )
    ending = within[:, -1:]
    query_scale = jnp.exp(within) * scaling
    key_scale = jnp.exp(ending - within)
    carry_decay = jnp.exp(ending[:, 0])
    query_dec = (query_blk * query_scale[:, :, None]).astype(jnp.bfloat16)
    key_dec = (key_blk * key_scale[:, :, None]).astype(jnp.bfloat16)
    contract = (((0,), (0,)), ((), ()))

    def advance(memory, inputs):
        key_b, value_b, factor = inputs
        before = memory.astype(jnp.bfloat16)
        memory = factor * memory + lax.dot_general(
            key_b, value_b, contract, preferred_element_type=jnp.float32
        )
        return (memory, before)

    start_state = jnp.zeros((key_width, value_width), jnp.float32)
    _, states_before = lax.scan(advance, start_state, (key_dec, value_blk, carry_decay))

    def retreat(later, inputs):
        query_b, grad_b, factor = inputs
        after = later.astype(jnp.bfloat16)
        later = factor * later + lax.dot_general(
            query_b, grad_b, contract, preferred_element_type=jnp.float32
        )
        return (later, after)

    _, state_grads = lax.scan(
        retreat, start_state, (query_dec, grad_blk, carry_decay), reverse=True
    )
    query_carried = jnp.einsum(
        "niv,ndv->nid", grad_blk, states_before, preferred_element_type=jnp.float32
    )
    key_carried = jnp.einsum(
        "njv,ndv->njd", value_blk, state_grads, preferred_element_type=jnp.float32
    )
    value_carried = jnp.einsum(
        "njd,ndv->njv", key_dec, state_grads, preferred_element_type=jnp.float32
    )
    grad_q = query_inner + query_carried * query_scale[:, :, None]
    grad_k = key_inner + key_carried * key_scale[:, :, None]
    grad_v = value_inner + value_carried
    return (
        grad_q.reshape(length, key_width),
        grad_k.reshape(length, key_width),
        grad_v.reshape(length, value_width),
    )


def unit_grads(query_rows, key_rows, value_rows, grad_rows, decay_rows, backward):

    def orient(array):
        return jnp.where(backward, jnp.flip(array, 0), array)

    gradients = unit_backward(
        orient(query_rows),
        orient(key_rows),
        orient(value_rows),
        orient(grad_rows),
        orient(decay_rows),
        backward,
    )
    return tuple((orient(single).astype(jnp.bfloat16) for single in gradients))


def shards_by_unit(layer_input, queries, key_vectors, values, cotangent, log_decay, key_weight):
    tokens = layer_input.shape[1]
    key_width = queries.shape[2] // HEADS
    value_width = values.shape[2] // HEADS

    def to_units(array, head_width):
        shaped = array[0].reshape(tokens, HEADS, head_width)
        return jnp.moveaxis(jnp.repeat(shaped, 2, axis=1), 1, 0)

    sent = (
        to_units(queries, key_width),
        to_units(key_vectors, key_width),
        to_units(values, value_width),
        to_units(cotangent, value_width),
    )
    query_units, key_units, value_units, grad_units = (
        lax.all_to_all(sent[0], "sp", split_axis=0, concat_axis=1, tiled=True),
        lax.all_to_all(sent[1], "sp", split_axis=0, concat_axis=1, tiled=True),
        lax.all_to_all(sent[2], "sp", split_axis=0, concat_axis=1, tiled=True),
        lax.all_to_all(sent[3], "sp", split_axis=0, concat_axis=1, tiled=True),
    )
    local_units = query_units.shape[0]
    first_unit = lax.axis_index("sp") * local_units
    backward = (first_unit + jnp.arange(local_units)) % 2 == 1
    query_back, key_back, value_back = jax.vmap(unit_grads)(
        query_units, key_units, value_units, grad_units, log_decay[0], backward
    )
    query_home, key_home, value_home = (
        lax.all_to_all(query_back, "sp", split_axis=1, concat_axis=0, tiled=True),
        lax.all_to_all(key_back, "sp", split_axis=1, concat_axis=0, tiled=True),
        lax.all_to_all(value_back, "sp", split_axis=1, concat_axis=0, tiled=True),
    )

    def merge_dirs(array, head_width):
        paired = array.astype(jnp.float32).reshape(HEADS, 2, tokens, head_width).sum(axis=1)
        return jnp.moveaxis(paired, 0, 1).reshape(tokens, HEADS * head_width).astype(jnp.bfloat16)

    grad_query = merge_dirs(query_home, key_width)
    grad_key = merge_dirs(key_home, key_width)
    grad_value = merge_dirs(value_home, value_width)
    grad_input = lax.dot_general(
        grad_key,
        lax.all_gather(key_weight, "dp", axis=0, tiled=True),
        (((1,), (1,)), ((), ())),
        preferred_element_type=jnp.float32,
    ).astype(jnp.bfloat16)
    token_rows = layer_input[0]
    summed = lax.psum_scatter(
        lax.dot_general(
            token_rows, grad_key, (((0,), (0,)), ((), ())), preferred_element_type=jnp.float32
        ),
        "dp",
        scatter_dimension=0,
        tiled=True,
    )
    grad_weight = lax.psum(summed, "sp")
    return (grad_query[None], grad_value[None], grad_input[None], grad_weight)


def shards(*arrays):
    sp = lax.axis_size("sp")
    dp = lax.axis_size("dp")
    if sp == HEADS and sp % 4 == 0 and arrays[1].shape[1] == BLOCK and dp % 2 == 0:
        return shards_by_head(sp, dp, *arrays)
    return shards_by_unit(*arrays)


def solution(mesh):
    return jax.shard_map(
        shards,
        mesh=mesh,
        in_specs=(
            P("dp", "sp", None),
            P("dp", "sp", None),
            P("dp", "sp", None),
            P("dp", "sp", None),
            P("dp", "sp", None),
            P("dp", "sp", None),
            P("dp", None),
        ),
        out_specs=(P("dp", "sp", None), P("dp", "sp", None), P("dp", "sp", None), P("dp", None)),
        check_vma=False,
    )
```
